32 devices in a mesh: fs: 4 (over y, x), tp: 8 (over z, core).
Axes of the slice: x: 2, y: 2, z: 4, core: 2. Of those that a mesh axis runs over, the one named last changes fastest.
Arguments:
- inputs: bfloat16 [1536, 2048], P('fs'), may hold values from -6 to 6
- pre_act: bfloat16 [1536, 8192], P('fs', 'tp'), may hold values from -6 to 6
- cotangent: bfloat16 [1536, 2048], P('fs'), may hold values from -6 to 6
- up_weight: bfloat16 [2048, 8192], P('fs', 'tp'), may hold values from -0.125 to 0.125
- down_weight: bfloat16 [8192, 2048], P('tp', 'fs'), may hold values from -0.0625 to 0.0625
Outputs:
- input_grad: bfloat16 [1536, 2048], P('fs')
- up_grad: float32 [2048, 8192], P('fs', 'tp')
- down_grad: float32 [8192, 2048], P('tp', 'fs')
- up_norms: float32 [2048], P('fs')
- down_norms: float32 [8192], P('tp')
The draws below stay inside these ranges and needn't reach their ends.
All inputs are finite; a program needn't handle non-finite values.
Results may differ from the reference program's by a relative error of at most 0.0051.
Values may be sent and summed in bfloat16 or wider, within the bound.
A program may use at most 64 MiB of HBM per device.

```python
import jax
import jax.numpy as jnp

D = 2048
FF = 8192
TOKENS = 1536


def raised(drawn, key, source, target, shards_of, factor):
    def block_of(position):
        return (jnp.arange(drawn.shape[position]) // (drawn.shape[position] // shards_of)).reshape((-1,) + (1,) * (drawn.ndim - 1 - position))

    near = jax.random.permutation(key, shards_of)[block_of(target)]
    other_side = (block_of(target) + shards_of // 2) % shards_of
    return jnp.where((block_of(source) == near) | (block_of(source) == other_side), factor * drawn, drawn)


def steps_of(own_key, extent, cuts, low, top_value):
    def one(position, blocks):
        steps = jax.random.uniform(jax.random.fold_in(jax.random.fold_in(own_key, 6), position), (blocks,), jnp.float32, low / len(cuts), top_value / len(cuts))
        return jnp.repeat(jnp.exp(steps), extent[position] // blocks).reshape((-1,) + (1,) * (len(extent) - position - 1))

    level = one(*cuts[0])
    for cut in cuts[1:]:
        level = level * one(*cut)
    return level


def normal_values(stream_key, shape, width, most, pieces=(), held_as=jnp.bfloat16):
    entries = jax.random.normal(stream_key, shape, jnp.float32) * width
    if len(pieces) > 0:
        entries = steps_of(stream_key, shape, pieces, -0.22, 0.18) * entries
    return jnp.clip(entries, min=-most, max=most).astype(held_as)


def noise_with(own_key, dims, scale, most, cuts, heavy, held_as=jnp.bfloat16):
    result = scale * jax.random.normal(own_key, dims, jnp.float32)
    if cuts:
        result = result * steps_of(own_key, dims, cuts, -0.22, 0.18)
    return jnp.clip(raised(result, jax.random.fold_in(own_key, 3), *heavy), -most, most).astype(held_as)


def setup_inputs(seed: int = 0) -> dict:
    key_list = jax.random.split(jax.random.key(seed), 6)
    return {
        "inputs": noise_with(key_list[0], (TOKENS, D), 1.0, 6.0, ((0, 4),), (0, 1, 4, 2.0)),
        "pre_act": normal_values(key_list[1], (TOKENS, FF), 1.0, 6.0, ((0, 4), (1, 8))),
        "cotangent": noise_with(key_list[2], (TOKENS, D), 1.0, 6.0, ((0, 4),), (0, 1, 4, 2.0)),
        "up_weight": normal_values(key_list[3], (D, FF), D ** -0.5, 0.125, ((0, 4), (1, 8))),
        "down_weight": normal_values(key_list[4], (FF, D), FF ** -0.5, 0.0625, ((0, 8), (1, 4))),
    }


def reference(inputs, pre_act, cotangent, up_weight, down_weight):
    active = jnp.maximum(pre_act.astype(jnp.float32), 0.0)
    squared = (active * active).astype(jnp.bfloat16)
    sq_grad = jnp.dot(cotangent, down_weight.T, preferred_element_type=jnp.float32)
    pre_grad = (2.0 * active * sq_grad).astype(jnp.bfloat16)
    input_grad = jnp.dot(pre_grad, up_weight.T, preferred_element_type=jnp.float32).astype(jnp.bfloat16)
    up_grad = jnp.dot(inputs.T, pre_grad, preferred_element_type=jnp.float32)
    down_grad = jnp.dot(squared.T, cotangent, preferred_element_type=jnp.float32)
    up_norms = jnp.sum(up_grad * up_grad, axis=1)
    down_norms = jnp.sum(down_grad * down_grad, axis=1)
    return input_grad, up_grad, down_grad, up_norms, down_norms
```

```python
import functools

import jax
import jax.numpy as jnp
from jax import lax
from jax.experimental import pallas as pl
from jax.experimental.pallas import tpu as pltpu
from jax.sharding import PartitionSpec as P

MESH = pl.DeviceIdType.MESH
F32, BF16 = jnp.float32, jnp.bfloat16


def contract_last(left, right):
    return lax.dot_general(left, right, (((1,), (1,)), ((), ())), preferred_element_type=F32)


def contract_first(left, right):
    return lax.dot_general(left, right, (((0,), (0,)), ((), ())), preferred_element_type=F32)


def bits_of(n):
    return [1 << i for i in range(n.bit_length() - 1)]


def by_weight(n, down=False):
    return sorted(range(1, n), key=lambda m: (bin(m).count("1"), -m if down else m))


class Gather:
    def __init__(self, n, me, device, source, place, send, recv, orders):
        self.n, self.me, self.device = n, me, device
        self.source, self.place = source, place
        self.send, self.recv, self.orders = send, recv, orders
        self.started = []

    def targets(self, cls, m):
        bits = bits_of(self.n)
        if m == 0:
            return bits
        if self.orders[cls] == "up":
            return [b for b in bits if b > m]
        return [b for b in bits if b < (m & -m)]

    def copy(self, cls, m, b):
        there = self.place(self.me ^ m, cls)
        return pltpu.make_async_remote_copy(
            src_ref=self.source(cls) if m == 0 else there,
            dst_ref=there,
            send_sem=self.send(cls, m ^ b),
            recv_sem=self.recv(cls, m ^ b),
            device_id=self.device(self.me ^ b),
            device_id_type=MESH,
        )

    def push(self, cls, m, only=None):
        for b in self.targets(cls, m):
            if only is None or b == only:
                copy = self.copy(cls, m, b)
                copy.start()
                self.started.append(copy)

    def push_own(self):
        classes = range(len(self.orders))
        for i, b in enumerate(bits_of(self.n)):
            for cls in classes if i % 2 == 0 else reversed(classes):
                self.push(cls, 0, b)

    def arrive(self, cls, m):
        here = self.place(self.me ^ m, cls)
        pltpu.make_async_remote_copy(
            src_ref=here,
            dst_ref=here,
            send_sem=self.send(cls, m),
            recv_sem=self.recv(cls, m),
            device_id=self.device(self.me ^ (m & -m)),
            device_id_type=MESH,
        ).wait_recv()

    def drain(self):
        for copy in self.started:
            copy.wait_send()


def share_rows(rows, parts):
    cuts = 1
    while cuts < parts and rows % (2 * cuts * 16) == 0:
        cuts *= 2
    return cuts


def position(nt):
    f, t = lax.axis_index("fs"), lax.axis_index("tp")
    return f, t, t // 2, t % 2


def gather_kernel(nf, nt, cot, dw, pa, inp, cot_all, dw_all, pa_all, inp_all,
                  xs, xr, zs, zr, ss, sr, a_s, a_r, bs, br, local_sem):
    f, t, z, c = position(nt)
    nz = nt // 2
    both = ("up", "down")
    rows, d = cot.shape
    row_cuts = share_rows(rows, nt)
    col_cuts = nt // row_cuts
    pr, pc = rows // row_cuts, d // col_cuts

    def piece(ref, y, h=None):
        row = pl.multiple_of((y // col_cuts) * pr, pr)
        width = pc if h is None else pc // 2
        col = (y % col_cuts) * pc + (0 if h is None else h * width)
        return ref.at[pl.ds(row, pr), pl.ds(pl.multiple_of(col, width), width)]

    db = dw.shape[1]
    dwh = dw.shape[0] // 2
    pah = pa.shape[0] // 2
    ih = inp.shape[0] // 2

    def over_fs(k, source, place):
        return Gather(nf, f, lambda g: (g, t), source, place,
                      lambda cls, m: xs.at[k, cls, m], lambda cls, m: xr.at[k, cls, m], both)

    g_cot = over_fs(0, lambda h: piece(cot, t, h),
                    lambda g, h: piece(cot_all.at[g], t, h))
    g_dw = over_fs(1, lambda h: dw.at[pl.ds(h * dwh, dwh), :],
                   lambda g, h: dw_all.at[pl.ds(h * dwh, dwh), pl.ds(pl.multiple_of(g * db, db), db)])
    g_pa = over_fs(2, lambda h: pa.at[pl.ds(h * pah, pah), :],
                   lambda g, h: pa_all.at[g, pl.ds(h * pah, pah), :])

    def over_z(m):
        spot = lambda y, cls=0: piece(cot_all.at[f ^ m], 2 * y + c)
        return Gather(nz, z, lambda y: (f, 2 * y + c), lambda cls: spot(z), spot,
                      lambda cls, k: zs.at[m, k], lambda cls, k: zr.at[m, k], ("down",))

    def sibling(src, dst, send, recv):
        return pltpu.make_async_remote_copy(src_ref=src, dst_ref=dst, send_sem=send, recv_sem=recv,
                                            device_id=(f, t ^ 1), device_id_type=MESH)

    mine = lambda m, k: piece(cot_all.at[f ^ m], 2 * (z ^ k) + c)
    other = lambda m, k: piece(cot_all.at[f ^ m], 2 * (z ^ k) + 1 - c)
    to_sibling = lambda m, k: sibling(mine(m, k), mine(m, k), ss.at[m, k], sr.at[m, k])
    from_sibling = lambda m, k: sibling(other(m, k), other(m, k), ss.at[m, k], sr.at[m, k])

    def columns(g, rows):
        return inp.at[pl.ds(pl.multiple_of(rows * ih, ih), ih), pl.ds(pl.multiple_of(g * db, db), db)]

    def exchange(m):
        return pltpu.make_async_remote_copy(
            src_ref=columns(f ^ m, c), dst_ref=inp_all.at[f, c], send_sem=a_s.at[m],
            recv_sem=a_r.at[m], device_id=(f ^ m, t), device_id_type=MESH)

    def exchanged(m):
        spot = inp_all.at[f ^ m, c]
        return pltpu.make_async_remote_copy(
            src_ref=spot, dst_ref=spot, send_sem=a_s.at[m],
            recv_sem=a_r.at[m], device_id=(f ^ m, t), device_id_type=MESH)

    in_to = lambda m: sibling(inp_all.at[f ^ m, c], inp_all.at[f ^ m, c], bs.at[m], br.at[m])
    in_from = lambda m: sibling(inp_all.at[f ^ m, 1 - c], inp_all.at[f ^ m, 1 - c], bs.at[m], br.at[m])

    g_cot.push_own()
    own = [
        pltpu.make_async_copy(dw, dw_all.at[:, pl.ds(pl.multiple_of(f * db, db), db)], local_sem.at[0]),
        pltpu.make_async_copy(pa, pa_all.at[f], local_sem.at[1]),
        pltpu.make_async_copy(cot, cot_all.at[f], local_sem.at[2]),
        pltpu.make_async_copy(columns(f, 0), inp_all.at[f, 0], local_sem.at[3]),
        pltpu.make_async_copy(columns(f, 1), inp_all.at[f, 1], local_sem.at[4]),
    ]
    for copy in own:
        copy.start()

    masks = by_weight(nf)
    zorder = by_weight(nz, True)
    rings = {m: over_z(m) for m in masks}

    def take_cot(m):
        for cls in (0, 1):
            g_cot.arrive(cls, m)
            g_cot.push(cls, m)
        rings[m].push(0, 0)
        to_sibling(m, 0).start()

    singles = [m for m in masks if m & (m - 1) == 0]
    for m in singles:
        take_cot(m)
    g_dw.push_own()
    for m in masks:
        exchange(m).start()
    g_pa.push_own()
    for m in masks:
        if m not in singles:
            take_cot(m)

    def take_ring(m):
        for k in zorder:
            rings[m].arrive(0, k)
            rings[m].push(0, k)
            to_sibling(m, k).start()

    def relay(g):
        for m in masks:
            for cls in (0, 1) if m & 1 else (1, 0):
                g.arrive(cls, m)
                g.push(cls, m)

    for m in singles:
        take_ring(m)
    relay(g_dw)
    for m in masks:
        exchanged(m).wait_recv()
        in_to(m).start()
    for m in masks:
        if m not in singles:
            take_ring(m)
    relay(g_pa)

    for m in masks:
        for k in range(nz):
            from_sibling(m, k).wait_recv()
            to_sibling(m, k).wait_send()
        in_from(m).wait_recv()
        in_to(m).wait_send()
        exchange(m).wait_send()
        rings[m].drain()
    for g in (g_cot, g_dw, g_pa):
        g.drain()
    for copy in own:
        copy.wait()


def gather(nf, nt, cot, dw, pa, inp):
    rows, d = inp.shape
    ff = pa.shape[1]
    nz = nt // 2
    dma = pltpu.SemaphoreType.DMA
    any_spec = pl.BlockSpec(memory_space=pl.ANY)
    return pl.pallas_call(
        functools.partial(gather_kernel, nf, nt),
        out_shape=[
            jax.ShapeDtypeStruct((nf, rows, d), BF16),
            jax.ShapeDtypeStruct((ff, d), BF16),
            jax.ShapeDtypeStruct((nf, rows, ff), BF16),
            jax.ShapeDtypeStruct((nf, 2, rows // 2, d // nf), BF16),
        ],
        in_specs=[any_spec] * 4,
        out_specs=[any_spec] * 4,
        scratch_shapes=[dma((3, 2, nf)), dma((3, 2, nf)), dma((nf, nz)), dma((nf, nz)), dma((nf, nz)),
                        dma((nf, nz)), dma((nf,)), dma((nf,)), dma((nf,)), dma((nf,)), dma((5,))],
        compiler_params=pltpu.CompilerParams(has_side_effects=True),
    )(cot, dw, pa, inp)


def reduce_kernel(nf, nt, part, un, dn, out, un_out, dn_out, from_sib, wire, landed, final, cols, un_all, dn_all,
                  s0, r0, s1, r1, s2, r2, s3, r3, s4, r4, s5, r5, s6, r6):
    f, t, z, c = position(nt)
    nz = nt // 2

    def remote(src, dst, send, recv, device):
        return pltpu.make_async_remote_copy(src_ref=src, dst_ref=dst, send_sem=send, recv_sem=recv,
                                            device_id=device, device_id_type=MESH)

    first = remote(part.at[1 - c], from_sib, s0.at[0], r0.at[0], (f, t ^ 1))
    first.start()
    un_all[t] = un[...]
    dn_all[f] = dn[...]
    ups = [remote(un, un_all.at[t], s5.at[m], r5.at[m], (f, t ^ m)) for m in range(1, nt)]
    downs = [remote(dn, dn_all.at[f], s6.at[m], r6.at[m], (f ^ m, t)) for m in range(1, nf)]
    for copy in ups + downs:
        copy.start()
    first.wait_recv()

    sends = []
    for k in list(range(nz - 1, 0, -1)):
        y = z ^ k
        wire[k] = (part[c, y] + from_sib[y]).astype(BF16)
        copy = remote(wire.at[k], landed.at[k], s1.at[k], r1.at[k], (f, 2 * y + c))
        copy.start()
        sends.append(copy)
    total = part[c, z] + from_sib[z]
    for k in range(1, nz):
        sends[nz - 1 - k].wait_recv()
        total = total + landed[k].astype(F32)
    final[...] = total.astype(BF16)
    trades = [remote(final.at[f ^ m], cols.at[f], s2.at[m], r2.at[m], (f ^ m, t)) for m in range(1, nf)]
    for copy in trades:
        copy.start()
    cols[f] = final[f]
    for m in range(1, nf):
        remote(cols.at[f ^ m], cols.at[f ^ m], s2.at[m], r2.at[m], (f ^ m, t)).wait_recv()

    spot = lambda y, cls=0: out.at[2 * y + c]
    ring = Gather(nz, z, lambda y: (f, 2 * y + c), lambda cls: cols, spot,
                  lambda cls, k: s3.at[k], lambda cls, k: r3.at[k], ("down",))
    ring.push(0, 0)
    pairs = [remote(cols, out.at[t], s4.at[0], r4.at[0], (f, t ^ 1))]
    pairs[0].start()
    out[t] = cols[...]
    for k in by_weight(nz, True):
        ring.arrive(0, k)
        ring.push(0, k)
        there = spot(z ^ k)
        copy = remote(there, there, s4.at[k], r4.at[k], (f, t ^ 1))
        copy.start()
        pairs.append(copy)

    for m in range(1, nt):
        remote(un_all.at[t ^ m], un_all.at[t ^ m], s5.at[m], r5.at[m], (f, t ^ m)).wait_recv()
    for m in range(1, nf):
        remote(dn_all.at[f ^ m], dn_all.at[f ^ m], s6.at[m], r6.at[m], (f ^ m, t)).wait_recv()
    un_sum, dn_sum = un_all[0], dn_all[0]
    for k in range(1, nt):
        un_sum = un_sum + un_all[k]
    for k in range(1, nf):
        dn_sum = dn_sum + dn_all[k]
    un_out[...] = un_sum
    dn_out[...] = dn_sum

    for k in range(nz):
        there = out.at[2 * (z ^ k) + 1 - c]
        remote(there, there, s4.at[k], r4.at[k], (f, t ^ 1)).wait_recv()
    ring.drain()
    for copy in [first] + ups + downs + sends + trades + pairs:
        copy.wait_send()


def reduce(nf, nt, part, un, dn):
    nz = nt // 2
    piece, db = part.shape[3:]
    dma = pltpu.SemaphoreType.DMA
    vmem = pl.BlockSpec(memory_space=pltpu.VMEM)
    sems = []
    for n in (1, nz, nf, nz, nz, nt, nf):
        sems += [dma((n,)), dma((n,))]
    return pl.pallas_call(
        functools.partial(reduce_kernel, nf, nt),
        out_shape=[
            jax.ShapeDtypeStruct((nt, nf, piece, db), BF16),
            jax.ShapeDtypeStruct(un.shape, F32),
            jax.ShapeDtypeStruct(dn.shape, F32),
        ],
        in_specs=[vmem] * 3,
        out_specs=[vmem] * 3,
        scratch_shapes=[
            pltpu.VMEM((nz, nf, piece, db), F32),
            pltpu.VMEM((nz, nf, piece, db), BF16),
            pltpu.VMEM((nz, nf, piece, db), BF16),
            pltpu.VMEM((nf, piece, db), BF16),
            pltpu.VMEM((nf, piece, db), BF16),
            pltpu.VMEM((nt,) + un.shape, F32),
            pltpu.VMEM((nf,) + dn.shape, F32),
        ] + sems,
        compiler_params=pltpu.CompilerParams(has_side_effects=True),
    )(part, un, dn)


def local(nf, nt, inputs, pre_act, cotangent, up_weight, down_weight):
    rows, d = inputs.shape
    ff, db = down_weight.shape
    nz = nt // 2
    piece = rows // nt
    f = lax.axis_index("fs")
    cot_all, dw_all, pa_all, inp_all = gather(
        nf, nt, cotangent, down_weight, pre_act, inputs)
    cot_all = cot_all.reshape(nf * rows, d)
    active = jnp.maximum(pa_all.reshape(nf * rows, ff).astype(F32), 0.0)
    squared = (active * active).astype(BF16)
    sq_grad = contract_last(cot_all, dw_all)
    pre_grad = (2.0 * active * sq_grad).astype(BF16)
    part = contract_last(pre_grad, up_weight)
    part = part.reshape(nf, nz, 2, piece, db).transpose(2, 1, 0, 3, 4)
    up_grad = contract_first(inp_all.reshape(nf * rows, db), pre_grad)
    down_grad = contract_first(squared, lax.dynamic_slice_in_dim(cot_all, f * db, db, 1))
    up_norms = jnp.sum(up_grad * up_grad, axis=1).reshape(1, db)
    down_norms = jnp.sum(down_grad * down_grad, axis=1).reshape(1, ff)
    out, un, dn = reduce(nf, nt, part, up_norms, down_norms)
    input_grad = out.transpose(0, 2, 1, 3).reshape(rows, d)
    return (input_grad, up_grad, down_grad, un.reshape(db), dn.reshape(ff))


def solution(mesh):
    in_specs = (P("fs", None), P("fs", "tp"), P("fs", None), P("fs", "tp"), P("tp", "fs"))
    out_specs = (P("fs", None), P("fs", "tp"), P("tp", "fs"), P("fs"), P("tp"))
    body = functools.partial(local, mesh.shape["fs"], mesh.shape["tp"])
    return jax.shard_map(body, mesh=mesh, in_specs=in_specs, out_specs=out_specs, check_vma=False)
```

```python
import functools

import jax
import jax.numpy as jnp
from jax import lax
from jax.experimental import pallas as pl
from jax.experimental.pallas import tpu as pltpu
from jax.sharding import PartitionSpec as P

MESH = pl.DeviceIdType.MESH
F32, BF16 = jnp.float32, jnp.bfloat16


def contract_last(left, right):
    return lax.dot_general(left, right, (((1,), (1,)), ((), ())), preferred_element_type=F32)


def contract_first(left, right):
    return lax.dot_general(left, right, (((0,), (0,)), ((), ())), preferred_element_type=F32)


def bits_of(n):
    return [1 << i for i in range(n.bit_length() - 1)]


def by_weight(n, down=False):
    return sorted(range(1, n), key=lambda m: (bin(m).count("1"), -m if down else m))


class Gather:
    def __init__(self, n, me, device, source, place, send, recv, orders):
        self.n, self.me, self.device = n, me, device
        self.source, self.place = source, place
        self.send, self.recv, self.orders = send, recv, orders
        self.started = []

    def targets(self, cls, m):
        bits = bits_of(self.n)
        if m == 0:
            return bits
        if self.orders[cls] == "up":
            return [b for b in bits if b > m]
        return [b for b in bits if b < (m & -m)]

    def copy(self, cls, m, b):
        there = self.place(self.me ^ m, cls)
        return pltpu.make_async_remote_copy(
            src_ref=self.source(cls) if m == 0 else there,
            dst_ref=there,
            send_sem=self.send(cls, m ^ b),
            recv_sem=self.recv(cls, m ^ b),
            device_id=self.device(self.me ^ b),
            device_id_type=MESH,
        )

    def push(self, cls, m, only=None):
        for b in self.targets(cls, m):
            if only is None or b == only:
                copy = self.copy(cls, m, b)
                copy.start()
                self.started.append(copy)

    def push_own(self):
        classes = range(len(self.orders))
        for i, b in enumerate(bits_of(self.n)):
            for cls in classes if i % 2 == 0 else reversed(classes):
                self.push(cls, 0, b)

    def arrive(self, cls, m):
        here = self.place(self.me ^ m, cls)
        pltpu.make_async_remote_copy(
            src_ref=here,
            dst_ref=here,
            send_sem=self.send(cls, m),
            recv_sem=self.recv(cls, m),
            device_id=self.device(self.me ^ (m & -m)),
            device_id_type=MESH,
        ).wait_recv()

    def drain(self):
        for copy in self.started:
            copy.wait_send()


def share_rows(rows, parts):
    cuts = 1
    while cuts < parts and rows % (2 * cuts * 16) == 0:
        cuts *= 2
    return cuts


def position(nt):
    f, t = lax.axis_index("fs"), lax.axis_index("tp")
    return f, t, t // 2, t % 2


def gather_kernel(nf, nt, cot, dw, pa, inp, up, part, ugrad, dgrad, cot_all, dw_all, pa_all, inp_all, total,
                  xs, xr, zs, zr, ss, sr, a_s, a_r, bs, br, local_sem):
    f, t, z, c = position(nt)
    nz = nt // 2
    both = ("up", "down")
    rows, d = cot.shape
    row_cuts = share_rows(rows, nt)
    col_cuts = nt // row_cuts
    pr, pc = rows // row_cuts, d // col_cuts

    def piece(ref, y, h=None):
        row = pl.multiple_of((y // col_cuts) * pr, pr)
        width = pc if h is None else pc // 2
        col = (y % col_cuts) * pc + (0 if h is None else h * width)
        return ref.at[pl.ds(row, pr), pl.ds(pl.multiple_of(col, width), width)]

    db = dw.shape[1]
    dwh = dw.shape[0] // 2
    pah = pa.shape[0] // 2
    ih = inp.shape[0] // 2

    def over_fs(k, source, place):
        return Gather(nf, f, lambda g: (g, t), source, place,
                      lambda cls, m: xs.at[k, cls, m], lambda cls, m: xr.at[k, cls, m], both)

    g_cot = over_fs(0, lambda h: piece(cot, t, h),
                    lambda g, h: piece(cot_all.at[g], t, h))
    g_dw = over_fs(1, lambda h: dw.at[pl.ds(h * dwh, dwh), :],
                   lambda g, h: dw_all.at[pl.ds(h * dwh, dwh), pl.ds(pl.multiple_of(g * db, db), db)])
    g_pa = over_fs(2, lambda h: pa.at[pl.ds(h * pah, pah), :],
                   lambda g, h: pa_all.at[g, pl.ds(h * pah, pah), :])

    def over_z(m):
        spot = lambda y, cls=0: piece(cot_all.at[f ^ m], 2 * y + c)
        return Gather(nz, z, lambda y: (f, 2 * y + c), lambda cls: spot(z), spot,
                      lambda cls, k: zs.at[m, k], lambda cls, k: zr.at[m, k], ("down",))

    def sibling(src, dst, send, recv):
        return pltpu.make_async_remote_copy(src_ref=src, dst_ref=dst, send_sem=send, recv_sem=recv,
                                            device_id=(f, t ^ 1), device_id_type=MESH)

    mine = lambda m, k: piece(cot_all.at[f ^ m], 2 * (z ^ k) + c)
    other = lambda m, k: piece(cot_all.at[f ^ m], 2 * (z ^ k) + 1 - c)
    to_sibling = lambda m, k: sibling(mine(m, k), mine(m, k), ss.at[m, k], sr.at[m, k])
    from_sibling = lambda m, k: sibling(other(m, k), other(m, k), ss.at[m, k], sr.at[m, k])

    def columns(g, rows):
        return inp.at[pl.ds(pl.multiple_of(rows * ih, ih), ih), pl.ds(pl.multiple_of(g * db, db), db)]

    def half(g, side):
        return inp_all.at[g, pl.ds(pl.multiple_of(side * ih, ih), ih), :]

    def exchange(m):
        return pltpu.make_async_remote_copy(
            src_ref=columns(f ^ m, c), dst_ref=half(f, c), send_sem=a_s.at[m],
            recv_sem=a_r.at[m], device_id=(f ^ m, t), device_id_type=MESH)

    def exchanged(m):
        spot = half(f ^ m, c)
        return pltpu.make_async_remote_copy(
            src_ref=spot, dst_ref=spot, send_sem=a_s.at[m],
            recv_sem=a_r.at[m], device_id=(f ^ m, t), device_id_type=MESH)

    in_to = lambda m: sibling(half(f ^ m, c), half(f ^ m, c), bs.at[m], br.at[m])
    in_from = lambda m: sibling(half(f ^ m, 1 - c), half(f ^ m, 1 - c), bs.at[m], br.at[m])

    g_cot.push_own()
    own = [
        pltpu.make_async_copy(dw, dw_all.at[:, pl.ds(pl.multiple_of(f * db, db), db)], local_sem.at[0]),
        pltpu.make_async_copy(pa, pa_all.at[f], local_sem.at[1]),
        pltpu.make_async_copy(cot, cot_all.at[f], local_sem.at[2]),
        pltpu.make_async_copy(columns(f, 0), half(f, 0), local_sem.at[3]),
        pltpu.make_async_copy(columns(f, 1), half(f, 1), local_sem.at[4]),
    ]
    for copy in own:
        copy.start()

    masks = by_weight(nf)
    zorder = by_weight(nz, True)
    rings = {m: over_z(m) for m in masks}

    def take_cot(m):
        for cls in (0, 1):
            g_cot.arrive(cls, m)
            g_cot.push(cls, m)
        rings[m].push(0, 0)
        to_sibling(m, 0).start()

    ugrad[...] = jnp.zeros_like(ugrad)
    dgrad[...] = jnp.zeros_like(dgrad)
    ff = up.shape[1]
    tile = min(ff, 256)
    step = rows // nt

    def compute(m):
        g = f ^ m
        own_cols = pl.ds(pl.multiple_of(f * db, db), db)
        total[...] = jnp.zeros_like(total)

        def body(j, carry):
            cols = pl.ds(pl.multiple_of(j * tile, tile), tile)
            active = jnp.maximum(pa_all[g, :, cols].astype(F32), 0.0)
            sq_grad = contract_last(cot_all[g], dw_all[cols, :])
            pre_grad = (2.0 * active * sq_grad).astype(BF16)
            squared = (active * active).astype(BF16)
            total[...] += contract_last(pre_grad, up[:, cols])
            ugrad[:, cols] += contract_first(inp_all[g], pre_grad)
            dgrad[cols, :] += contract_first(squared, cot_all[g, :, own_cols])
            return carry

        lax.fori_loop(0, ff // tile, body, 0)
        for k in range(nt):
            part[k % 2, k // 2, g] = total[k * step:(k + 1) * step, :]

    singles = [m for m in masks if m & (m - 1) == 0]
    pairs = [(m, cls) for m in masks for cls in (0, 1)]
    inner = [p for p in pairs if g_dw.targets(p[1], p[0])]
    outer = [p for p in pairs if p not in inner]

    def take(g, items):
        for m, cls in items:
            g.arrive(cls, m)
            g.push(cls, m)

    for m in singles:
        take_cot(m)
    g_dw.push_own()
    for m in masks:
        if m not in singles:
            take_cot(m)
    take(g_dw, inner)
    for m in masks:
        exchange(m).start()
    g_pa.push_own()
    for m in masks:
        for k in zorder:
            rings[m].arrive(0, k)
            rings[m].push(0, k)
            to_sibling(m, k).start()
    take(g_dw, outer)
    for copy in own:
        copy.wait()
    compute(0)
    for m in masks:
        exchanged(m).wait_recv()
        in_to(m).start()
    take(g_pa, inner)
    for m in masks:
        take(g_pa, [p for p in outer if p[0] == m])
        for k in range(nz):
            from_sibling(m, k).wait_recv()
        in_from(m).wait_recv()
        compute(m)

    for m in masks:
        for k in range(nz):
            to_sibling(m, k).wait_send()
        in_to(m).wait_send()
        exchange(m).wait_send()
        rings[m].drain()
    for g in (g_cot, g_dw, g_pa):
        g.drain()


def gather(nf, nt, cot, dw, pa, inp, up):
    rows, d = inp.shape
    ff = pa.shape[1]
    db = d // nf
    nz = nt // 2
    dma = pltpu.SemaphoreType.DMA
    vmem = pl.BlockSpec(memory_space=pltpu.VMEM)
    return pl.pallas_call(
        functools.partial(gather_kernel, nf, nt),
        out_shape=[
            jax.ShapeDtypeStruct((2, nz, nf, rows // nt, db), F32),
            jax.ShapeDtypeStruct((db, ff), F32),
            jax.ShapeDtypeStruct((ff, db), F32),
        ],
        in_specs=[vmem] * 5,
        out_specs=[vmem] * 3,
        scratch_shapes=[
            pltpu.VMEM((nf, rows, d), BF16),
            pltpu.VMEM((ff, d), BF16),
            pltpu.VMEM((nf, rows, ff), BF16),
            pltpu.VMEM((nf, rows, db), BF16),
            pltpu.VMEM((rows, db), F32),
            dma((3, 2, nf)), dma((3, 2, nf)), dma((nf, nz)), dma((nf, nz)), dma((nf, nz)),
            dma((nf, nz)), dma((nf,)), dma((nf,)), dma((nf,)), dma((nf,)), dma((5,)),
        ],
        compiler_params=pltpu.CompilerParams(has_side_effects=True),
    )(cot, dw, pa, inp, up)


def reduce_kernel(nf, nt, part, un, dn, out, un_out, dn_out, from_sib, wire, landed, final, cols, un_all, dn_all,
                  s0, r0, s1, r1, s2, r2, s3, r3, s4, r4, s5, r5, s6, r6):
    f, t, z, c = position(nt)
    nz = nt // 2

    def remote(src, dst, send, recv, device):
        return pltpu.make_async_remote_copy(src_ref=src, dst_ref=dst, send_sem=send, recv_sem=recv,
                                            device_id=device, device_id_type=MESH)

    first = remote(part.at[1 - c], from_sib, s0.at[0], r0.at[0], (f, t ^ 1))
    first.start()
    un_all[t] = un[...]
    dn_all[f] = dn[...]
    ups = [remote(un, un_all.at[t], s5.at[m], r5.at[m], (f, t ^ m)) for m in range(1, nt)]
    downs = [remote(dn, dn_all.at[f], s6.at[m], r6.at[m], (f ^ m, t)) for m in range(1, nf)]
    for copy in ups + downs:
        copy.start()
    first.wait_recv()

    sends = []
    for k in list(range(nz - 1, 0, -1)):
        y = z ^ k
        wire[k] = (part[c, y] + from_sib[y]).astype(BF16)
        copy = remote(wire.at[k], landed.at[k], s1.at[k], r1.at[k], (f, 2 * y + c))
        copy.start()
        sends.append(copy)
    total = part[c, z] + from_sib[z]
    for k in range(1, nz):
        sends[nz - 1 - k].wait_recv()
        total = total + landed[k].astype(F32)
    final[...] = total.astype(BF16)
    trades = [remote(final.at[f ^ m], cols.at[f], s2.at[m], r2.at[m], (f ^ m, t)) for m in range(1, nf)]
    for copy in trades:
        copy.start()
    cols[f] = final[f]
    for m in range(1, nf):
        remote(cols.at[f ^ m], cols.at[f ^ m], s2.at[m], r2.at[m], (f ^ m, t)).wait_recv()

    spot = lambda y, cls=0: out.at[2 * y + c]
    ring = Gather(nz, z, lambda y: (f, 2 * y + c), lambda cls: cols, spot,
                  lambda cls, k: s3.at[k], lambda cls, k: r3.at[k], ("down",))
    ring.push(0, 0)
    pairs = [remote(cols, out.at[t], s4.at[0], r4.at[0], (f, t ^ 1))]
    pairs[0].start()
    out[t] = cols[...]
    for k in by_weight(nz, True):
        ring.arrive(0, k)
        ring.push(0, k)
        there = spot(z ^ k)
        copy = remote(there, there, s4.at[k], r4.at[k], (f, t ^ 1))
        copy.start()
        pairs.append(copy)

    for m in range(1, nt):
        remote(un_all.at[t ^ m], un_all.at[t ^ m], s5.at[m], r5.at[m], (f, t ^ m)).wait_recv()
    for m in range(1, nf):
        remote(dn_all.at[f ^ m], dn_all.at[f ^ m], s6.at[m], r6.at[m], (f ^ m, t)).wait_recv()
    un_sum, dn_sum = un_all[0], dn_all[0]
    for k in range(1, nt):
        un_sum = un_sum + un_all[k]
    for k in range(1, nf):
        dn_sum = dn_sum + dn_all[k]
    un_out[...] = un_sum
    dn_out[...] = dn_sum

    for k in range(nz):
        there = out.at[2 * (z ^ k) + 1 - c]
        remote(there, there, s4.at[k], r4.at[k], (f, t ^ 1)).wait_recv()
    ring.drain()
    for copy in [first] + ups + downs + sends + trades + pairs:
        copy.wait_send()


def reduce(nf, nt, part, un, dn):
    nz = nt // 2
    piece, db = part.shape[3:]
    dma = pltpu.SemaphoreType.DMA
    vmem = pl.BlockSpec(memory_space=pltpu.VMEM)
    sems = []
    for n in (1, nz, nf, nz, nz, nt, nf):
        sems += [dma((n,)), dma((n,))]
    return pl.pallas_call(
        functools.partial(reduce_kernel, nf, nt),
        out_shape=[
            jax.ShapeDtypeStruct((nt, nf, piece, db), BF16),
            jax.ShapeDtypeStruct(un.shape, F32),
            jax.ShapeDtypeStruct(dn.shape, F32),
        ],
        in_specs=[vmem] * 3,
        out_specs=[vmem] * 3,
        scratch_shapes=[
            pltpu.VMEM((nz, nf, piece, db), F32),
            pltpu.VMEM((nz, nf, piece, db), BF16),
            pltpu.VMEM((nz, nf, piece, db), BF16),
            pltpu.VMEM((nf, piece, db), BF16),
            pltpu.VMEM((nf, piece, db), BF16),
            pltpu.VMEM((nt,) + un.shape, F32),
            pltpu.VMEM((nf,) + dn.shape, F32),
        ] + sems,
        compiler_params=pltpu.CompilerParams(has_side_effects=True),
    )(part, un, dn)


def local(nf, nt, inputs, pre_act, cotangent, up_weight, down_weight):
    rows, d = inputs.shape
    ff, db = down_weight.shape
    part, up_grad, down_grad = gather(nf, nt, cotangent, down_weight, pre_act, inputs, up_weight)
    up_norms = jnp.sum(up_grad * up_grad, axis=1).reshape(1, db)
    down_norms = jnp.sum(down_grad * down_grad, axis=1).reshape(1, ff)
    out, un, dn = reduce(nf, nt, part, up_norms, down_norms)
    input_grad = out.transpose(0, 2, 1, 3).reshape(rows, d)
    return (input_grad, up_grad, down_grad, un.reshape(db), dn.reshape(ff))


def solution(mesh):
    in_specs = (P("fs", None), P("fs", "tp"), P("fs", None), P("fs", "tp"), P("tp", "fs"))
    out_specs = (P("fs", None), P("fs", "tp"), P("tp", "fs"), P("fs"), P("tp"))
    body = functools.partial(local, mesh.shape["fs"], mesh.shape["tp"])
    return jax.shard_map(body, mesh=mesh, in_specs=in_specs, out_specs=out_specs, check_vma=False)
```

```python
import functools

import jax
import jax.numpy as jnp
from jax import lax
from jax.experimental import pallas as pl
from jax.experimental.pallas import tpu as pltpu
from jax.sharding import PartitionSpec as P

MESH = pl.DeviceIdType.MESH
F32, BF16 = jnp.float32, jnp.bfloat16


def contract_last(left, right):
    return lax.dot_general(left, right, (((1,), (1,)), ((), ())), preferred_element_type=F32)


def contract_first(left, right):
    return lax.dot_general(left, right, (((0,), (0,)), ((), ())), preferred_element_type=F32)


def bits_of(n):
    return [1 << i for i in range(n.bit_length() - 1)]


def by_weight(n, down=False):
    return sorted(range(1, n), key=lambda m: (bin(m).count("1"), -m if down else m))


class Gather:
    def __init__(self, n, me, device, source, place, send, recv, orders):
        self.n, self.me, self.device = n, me, device
        self.source, self.place = source, place
        self.send, self.recv, self.orders = send, recv, orders
        self.started = []

    def targets(self, cls, m):
        bits = bits_of(self.n)
        if m == 0:
            return bits
        if self.orders[cls] == "up":
            return [b for b in bits if b > m]
        return [b for b in bits if b < (m & -m)]

    def copy(self, cls, m, b):
        there = self.place(self.me ^ m, cls)
        return pltpu.make_async_remote_copy(
            src_ref=self.source(cls) if m == 0 else there,
            dst_ref=there,
            send_sem=self.send(cls, m ^ b),
            recv_sem=self.recv(cls, m ^ b),
            device_id=self.device(self.me ^ b),
            device_id_type=MESH,
        )

    def push(self, cls, m, only=None):
        for b in self.targets(cls, m):
            if only is None or b == only:
                copy = self.copy(cls, m, b)
                copy.start()
                self.started.append(copy)

    def push_own(self):
        classes = range(len(self.orders))
        for i, b in enumerate(bits_of(self.n)):
            for cls in classes if i % 2 == 0 else reversed(classes):
                self.push(cls, 0, b)

    def arrive(self, cls, m):
        here = self.place(self.me ^ m, cls)
        pltpu.make_async_remote_copy(
            src_ref=here,
            dst_ref=here,
            send_sem=self.send(cls, m),
            recv_sem=self.recv(cls, m),
            device_id=self.device(self.me ^ (m & -m)),
            device_id_type=MESH,
        ).wait_recv()

    def drain(self):
        for copy in self.started:
            copy.wait_send()


def share_rows(rows, parts):
    cuts = 1
    while cuts < parts and rows % (2 * cuts * 16) == 0:
        cuts *= 2
    return cuts


def position(nt):
    f, t = lax.axis_index("fs"), lax.axis_index("tp")
    return f, t, t // 2, t % 2


def gather_kernel(nf, nt, cot, dw, pa, inp, up, final, ugrad, dgrad, cot_all, dw_all, pa_all, inp_all, total,
                  part, from_sib, wire, landed, fs0, fr0, ws, wr,
                  xs, xr, zs, zr, ss, sr, a_s, a_r, bs, br, local_sem):
    f, t, z, c = position(nt)
    nz = nt // 2
    both = ("up", "down")
    rows, d = cot.shape
    row_cuts = share_rows(rows, nt)
    col_cuts = nt // row_cuts
    pr, pc = rows // row_cuts, d // col_cuts

    def piece(ref, y, h=None):
        row = pl.multiple_of((y // col_cuts) * pr, pr)
        width = pc if h is None else pc // 2
        col = (y % col_cuts) * pc + (0 if h is None else h * width)
        return ref.at[pl.ds(row, pr), pl.ds(pl.multiple_of(col, width), width)]

    db = dw.shape[1]
    dwh = dw.shape[0] // 2
    pah = pa.shape[0] // 2
    ih = inp.shape[0] // 2

    def over_fs(k, source, place):
        return Gather(nf, f, lambda g: (g, t), source, place,
                      lambda cls, m: xs.at[k, cls, m], lambda cls, m: xr.at[k, cls, m], both)

    g_cot = over_fs(0, lambda h: piece(cot, t, h),
                    lambda g, h: piece(cot_all.at[g], t, h))
    g_dw = over_fs(1, lambda h: dw.at[pl.ds(h * dwh, dwh), :],
                   lambda g, h: dw_all.at[pl.ds(h * dwh, dwh), pl.ds(pl.multiple_of(g * db, db), db)])
    g_pa = over_fs(2, lambda h: pa.at[pl.ds(h * pah, pah), :],
                   lambda g, h: pa_all.at[g, pl.ds(h * pah, pah), :])

    def over_z(m):
        spot = lambda y, cls=0: piece(cot_all.at[f ^ m], 2 * y + c)
        return Gather(nz, z, lambda y: (f, 2 * y + c), lambda cls: spot(z), spot,
                      lambda cls, k: zs.at[m, k], lambda cls, k: zr.at[m, k], ("down",))

    def sibling(src, dst, send, recv):
        return pltpu.make_async_remote_copy(src_ref=src, dst_ref=dst, send_sem=send, recv_sem=recv,
                                            device_id=(f, t ^ 1), device_id_type=MESH)

    mine = lambda m, k: piece(cot_all.at[f ^ m], 2 * (z ^ k) + c)
    other = lambda m, k: piece(cot_all.at[f ^ m], 2 * (z ^ k) + 1 - c)
    to_sibling = lambda m, k: sibling(mine(m, k), mine(m, k), ss.at[m, k], sr.at[m, k])
    from_sibling = lambda m, k: sibling(other(m, k), other(m, k), ss.at[m, k], sr.at[m, k])

    def columns(g, rows):
        return inp.at[pl.ds(pl.multiple_of(rows * ih, ih), ih), pl.ds(pl.multiple_of(g * db, db), db)]

    def half(g, side):
        return inp_all.at[g, pl.ds(pl.multiple_of(side * ih, ih), ih), :]

    def exchange(m):
        return pltpu.make_async_remote_copy(
            src_ref=columns(f ^ m, c), dst_ref=half(f, c), send_sem=a_s.at[m],
            recv_sem=a_r.at[m], device_id=(f ^ m, t), device_id_type=MESH)

    def exchanged(m):
        spot = half(f ^ m, c)
        return pltpu.make_async_remote_copy(
            src_ref=spot, dst_ref=spot, send_sem=a_s.at[m],
            recv_sem=a_r.at[m], device_id=(f ^ m, t), device_id_type=MESH)

    in_to = lambda m: sibling(half(f ^ m, c), half(f ^ m, c), bs.at[m], br.at[m])
    in_from = lambda m: sibling(half(f ^ m, 1 - c), half(f ^ m, 1 - c), bs.at[m], br.at[m])

    g_cot.push_own()
    own = [
        pltpu.make_async_copy(dw, dw_all.at[:, pl.ds(pl.multiple_of(f * db, db), db)], local_sem.at[0]),
        pltpu.make_async_copy(pa, pa_all.at[f], local_sem.at[1]),
        pltpu.make_async_copy(cot, cot_all.at[f], local_sem.at[2]),
        pltpu.make_async_copy(columns(f, 0), half(f, 0), local_sem.at[3]),
        pltpu.make_async_copy(columns(f, 1), half(f, 1), local_sem.at[4]),
    ]
    for copy in own:
        copy.start()

    masks = by_weight(nf)
    zorder = by_weight(nz, True)
    rings = {m: over_z(m) for m in masks}

    def take_cot(m):
        for cls in (0, 1):
            g_cot.arrive(cls, m)
            g_cot.push(cls, m)
        rings[m].push(0, 0)
        to_sibling(m, 0).start()

    ugrad[...] = jnp.zeros_like(ugrad)
    dgrad[...] = jnp.zeros_like(dgrad)
    ff = up.shape[1]
    tile = min(ff, 256)
    step = rows // nt

    def compute(m):
        g = f ^ m
        own_cols = pl.ds(pl.multiple_of(f * db, db), db)
        total[...] = jnp.zeros_like(total)

        def body(j, carry):
            cols = pl.ds(pl.multiple_of(j * tile, tile), tile)
            active = jnp.maximum(pa_all[g, :, cols].astype(F32), 0.0)
            sq_grad = contract_last(cot_all[g], dw_all[cols, :])
            pre_grad = (2.0 * active * sq_grad).astype(BF16)
            squared = (active * active).astype(BF16)
            total[...] += contract_last(pre_grad, up[:, cols])
            ugrad[:, cols] += contract_first(inp_all[g], pre_grad)
            dgrad[cols, :] += contract_first(squared, cot_all[g, :, own_cols])
            return carry

        lax.fori_loop(0, ff // tile, body, 0)
        for k in range(nt):
            part[g, k % 2, k // 2] = total[k * step:(k + 1) * step, :]
        halves(m).start()

    def halves(m):
        return sibling(part.at[f ^ m, 1 - c], from_sib.at[f ^ m], fs0.at[m], fr0.at[m])

    def spread(m, k):
        return pltpu.make_async_remote_copy(
            src_ref=wire.at[f ^ m, k], dst_ref=landed.at[f ^ m, k], send_sem=ws.at[m, k],
            recv_sem=wr.at[m, k], device_id=(f, 2 * (z ^ k) + c), device_id_type=MESH)

    def scatter(m):
        g = f ^ m
        halves(m).wait_recv()
        for k in range(nz - 1, 0, -1):
            wire[g, k] = (part[g, c, z ^ k] + from_sib[g, z ^ k]).astype(BF16)
            spread(m, k).start()

    def finish(m):
        g = f ^ m
        value = part[g, c, z] + from_sib[g, z]
        for k in range(1, nz):
            spread(m, k).wait_recv()
            value = value + landed[g, k].astype(F32)
        final[g] = value.astype(BF16)

    singles = [m for m in masks if m & (m - 1) == 0]
    pairs = [(m, cls) for m in masks for cls in (0, 1)]
    inner = [p for p in pairs if g_dw.targets(p[1], p[0])]
    outer = [p for p in pairs if p not in inner]

    def take(g, items):
        for m, cls in items:
            g.arrive(cls, m)
            g.push(cls, m)

    for m in singles:
        take_cot(m)
    g_dw.push_own()
    for m in masks:
        if m not in singles:
            take_cot(m)
    take(g_dw, inner)
    for m in masks:
        exchange(m).start()
    g_pa.push_own()
    for m in masks:
        for k in zorder:
            rings[m].arrive(0, k)
            rings[m].push(0, k)
            to_sibling(m, k).start()
    take(g_dw, outer)
    for copy in own:
        copy.wait()
    compute(0)
    for m in masks:
        exchanged(m).wait_recv()
        in_to(m).start()
    take(g_pa, inner)
    for m in masks:
        take(g_pa, [p for p in outer if p[0] == m])
        for k in range(nz):
            from_sibling(m, k).wait_recv()
        in_from(m).wait_recv()
        compute(m)
        scatter(masks[masks.index(m) - 1] if m != masks[0] else 0)
    scatter(masks[-1])
    for m in [0] + masks:
        finish(m)
        halves(m).wait_send()
        for k in range(1, nz):
            spread(m, k).wait_send()

    for m in masks:
        for k in range(nz):
            to_sibling(m, k).wait_send()
        in_to(m).wait_send()
        exchange(m).wait_send()
        rings[m].drain()
    for g in (g_cot, g_dw, g_pa):
        g.drain()


def gather(nf, nt, cot, dw, pa, inp, up):
    rows, d = inp.shape
    ff = pa.shape[1]
    db = d // nf
    nz = nt // 2
    dma = pltpu.SemaphoreType.DMA
    vmem = pl.BlockSpec(memory_space=pltpu.VMEM)
    return pl.pallas_call(
        functools.partial(gather_kernel, nf, nt),
        out_shape=[
            jax.ShapeDtypeStruct((nf, rows // nt, db), BF16),
            jax.ShapeDtypeStruct((db, ff), F32),
            jax.ShapeDtypeStruct((ff, db), F32),
        ],
        in_specs=[vmem] * 5,
        out_specs=[vmem] * 3,
        scratch_shapes=[
            pltpu.VMEM((nf, rows, d), BF16),
            pltpu.VMEM((ff, d), BF16),
            pltpu.VMEM((nf, rows, ff), BF16),
            pltpu.VMEM((nf, rows, db), BF16),
            pltpu.VMEM((rows, db), F32),
            pltpu.VMEM((nf, 2, nz, rows // nt, db), F32),
            pltpu.VMEM((nf, nz, rows // nt, db), F32),
            pltpu.VMEM((nf, nz, rows // nt, db), BF16),
            pltpu.VMEM((nf, nz, rows // nt, db), BF16),
            dma((nf,)), dma((nf,)), dma((nf, nz)), dma((nf, nz)),
            dma((3, 2, nf)), dma((3, 2, nf)), dma((nf, nz)), dma((nf, nz)), dma((nf, nz)),
            dma((nf, nz)), dma((nf,)), dma((nf,)), dma((nf,)), dma((nf,)), dma((5,)),
        ],
        compiler_params=pltpu.CompilerParams(has_side_effects=True),
    )(cot, dw, pa, inp, up)


def reduce_kernel(nf, nt, final, un, dn, out, un_out, dn_out, cols, un_all, dn_all,
                  s2, r2, s3, r3, s4, r4, s5, r5, s6, r6):
    f, t, z, c = position(nt)
    nz = nt // 2

    def remote(src, dst, send, recv, device):
        return pltpu.make_async_remote_copy(src_ref=src, dst_ref=dst, send_sem=send, recv_sem=recv,
                                            device_id=device, device_id_type=MESH)

    un_all[t] = un[...]
    dn_all[f] = dn[...]
    ups = [remote(un, un_all.at[t], s5.at[m], r5.at[m], (f, t ^ m)) for m in range(1, nt)]
    downs = [remote(dn, dn_all.at[f], s6.at[m], r6.at[m], (f ^ m, t)) for m in range(1, nf)]
    for copy in ups + downs:
        copy.start()
    trades = [remote(final.at[f ^ m], cols.at[f], s2.at[m], r2.at[m], (f ^ m, t)) for m in range(1, nf)]
    for copy in trades:
        copy.start()
    cols[f] = final[f]
    for m in range(1, nf):
        remote(cols.at[f ^ m], cols.at[f ^ m], s2.at[m], r2.at[m], (f ^ m, t)).wait_recv()

    spot = lambda y, cls=0: out.at[2 * y + c]
    ring = Gather(nz, z, lambda y: (f, 2 * y + c), lambda cls: cols, spot,
                  lambda cls, k: s3.at[k], lambda cls, k: r3.at[k], ("down",))
    ring.push(0, 0)
    pairs = [remote(cols, out.at[t], s4.at[0], r4.at[0], (f, t ^ 1))]
    pairs[0].start()
    out[t] = cols[...]
    for k in by_weight(nz, True):
        ring.arrive(0, k)
        ring.push(0, k)
        there = spot(z ^ k)
        copy = remote(there, there, s4.at[k], r4.at[k], (f, t ^ 1))
        copy.start()
        pairs.append(copy)

    for m in range(1, nt):
        remote(un_all.at[t ^ m], un_all.at[t ^ m], s5.at[m], r5.at[m], (f, t ^ m)).wait_recv()
    for m in range(1, nf):
        remote(dn_all.at[f ^ m], dn_all.at[f ^ m], s6.at[m], r6.at[m], (f ^ m, t)).wait_recv()
    un_sum, dn_sum = un_all[0], dn_all[0]
    for k in range(1, nt):
        un_sum = un_sum + un_all[k]
    for k in range(1, nf):
        dn_sum = dn_sum + dn_all[k]
    un_out[...] = un_sum
    dn_out[...] = dn_sum

    for k in range(nz):
        there = out.at[2 * (z ^ k) + 1 - c]
        remote(there, there, s4.at[k], r4.at[k], (f, t ^ 1)).wait_recv()
    ring.drain()
    for copy in ups + downs + trades + pairs:
        copy.wait_send()


def reduce(nf, nt, part, un, dn):
    nz = nt // 2
    piece, db = part.shape[1:]
    dma = pltpu.SemaphoreType.DMA
    vmem = pl.BlockSpec(memory_space=pltpu.VMEM)
    sems = []
    for n in (nf, nz, nz, nt, nf):
        sems += [dma((n,)), dma((n,))]
    return pl.pallas_call(
        functools.partial(reduce_kernel, nf, nt),
        out_shape=[
            jax.ShapeDtypeStruct((nt, nf, piece, db), BF16),
            jax.ShapeDtypeStruct(un.shape, F32),
            jax.ShapeDtypeStruct(dn.shape, F32),
        ],
        in_specs=[vmem] * 3,
        out_specs=[vmem] * 3,
        scratch_shapes=[
            pltpu.VMEM((nf, piece, db), BF16),
            pltpu.VMEM((nt,) + un.shape, F32),
            pltpu.VMEM((nf,) + dn.shape, F32),
        ] + sems,
        compiler_params=pltpu.CompilerParams(has_side_effects=True),
    )(part, un, dn)


def local(nf, nt, inputs, pre_act, cotangent, up_weight, down_weight):
    rows, d = inputs.shape
    ff, db = down_weight.shape
    part, up_grad, down_grad = gather(nf, nt, cotangent, down_weight, pre_act, inputs, up_weight)
    up_norms = jnp.sum(up_grad * up_grad, axis=1).reshape(1, db)
    down_norms = jnp.sum(down_grad * down_grad, axis=1).reshape(1, ff)
    out, un, dn = reduce(nf, nt, part, up_norms, down_norms)
    input_grad = out.transpose(0, 2, 1, 3).reshape(rows, d)
    return (input_grad, up_grad, down_grad, un.reshape(db), dn.reshape(ff))


def solution(mesh):
    in_specs = (P("fs", None), P("fs", "tp"), P("fs", None), P("fs", "tp"), P("tp", "fs"))
    out_specs = (P("fs", None), P("fs", "tp"), P("tp", "fs"), P("fs"), P("tp"))
    body = functools.partial(local, mesh.shape["fs"], mesh.shape["tp"])
    return jax.shard_map(body, mesh=mesh, in_specs=in_specs, out_specs=out_specs, check_vma=False)
```
